32 devices in a mesh: sp: 8 (over z, y), tp: 4 (over x, core).
Axes of the slice: x: 2, y: 2, z: 4, core: 2. Of those that a mesh axis runs over, the one named last changes fastest.
Arguments:
- inputs: bfloat16 [8192, 2048], P('sp'), may hold values from -6 to 6
- norm_gain: float32 [3, 2048], replicated, may hold values from 0.1 to 1.9
- query_weight: bfloat16 [3, 2048, 1024], P(None, 'sp', 'tp'), may hold values from -64 to 64
- key_weight: bfloat16 [3, 2048, 512], P(None, 'sp', 'tp'), may hold values from -4 to 4
- value_weight: bfloat16 [3, 2048, 512], P(None, 'sp', 'tp'), may hold values from -0.125 to 0.125
- output_weight: bfloat16 [3, 2048, 1024], P(None, 'sp', 'tp'), may hold values from -0.1875 to 0.1875
- sink_logit: float32 [3, 16], P(None, 'tp'), may hold values from 2 to 7
- final_gain: float32 [2048], replicated, may hold values from 0.1 to 1.9
Outputs:
- result: float32 [8192, 2048], P(('sp', 'tp'))
The draws below stay inside these ranges and needn't reach their ends.
All inputs are finite; a program needn't handle non-finite values.
Results may differ from the reference program's by a relative error of at most 0.015.
Values may be sent and summed in bfloat16 or wider, within the bound.
A program may use at most 64 MiB of HBM per device.

```python
import jax
import jax.numpy as jnp
from jax import lax

D = 2048
HEADS = 16
KV_HEADS = 8
HEAD_DIM = 64
WINDOW = 128
LAYERS = 3
TOK_DEV = 1024
SEQ = 8192


def shared_keys(key):
    base_key = jax.random.fold_in(key, 7)
    shape = (LAYERS, D, KV_HEADS * HEAD_DIM)
    return jnp.clip(jax.random.normal(base_key, shape, jnp.float32), -4.0, 4.0)


def draw_key_weight(key, part):
    return shared_keys(key).astype(jnp.bfloat16)


def draw_query_weight(key, part):
    base_key = jax.random.fold_in(key, 13)
    drawn = jax.random.normal(base_key, (LAYERS, D, HEADS * HEAD_DIM), jnp.float32)
    return jnp.clip(drawn, -4.0, 4.0).astype(jnp.bfloat16)


def level_of(key, dims, shards, smallest, high):
    loudness = 1.0
    for position, parts in shards:
        draws = jax.random.uniform(jax.random.fold_in(jax.random.fold_in(key, 6), position), (parts,), jnp.float32, smallest / len(shards), high / len(shards))
        loudness = loudness * jnp.repeat(jnp.exp(draws), dims[position] // parts).reshape((-1,) + (1,) * (len(dims) - 1 - position))
    return loudness


def bell_draw(own_key, extent, deviation, bound, cuts=(), kind=jnp.bfloat16):
    values = jax.random.normal(own_key, extent, jnp.float32) * deviation
    if len(cuts) > 0:
        values = level_of(own_key, extent, cuts, -0.22, 0.18) * values
    return jnp.clip(values, min=-bound, max=bound).astype(kind)


def setup_inputs(seed: int = 0) -> dict:
    streams_of = jax.random.split(jax.random.key(seed), 9)
    inputs = bell_draw(streams_of[0], (SEQ, D), 1.0, 6.0, ((0, 8),))
    norm_gain = jnp.clip(1.0 + 0.18 * jax.random.normal(streams_of[1], (LAYERS, D), jnp.float32), 0.1, 1.9)
    query_weight = draw_query_weight(jax.random.fold_in(streams_of[8], 71), 0)
    key_weight = draw_key_weight(jax.random.fold_in(streams_of[8], 71), 0)
    value_weight = bell_draw(streams_of[4], (LAYERS, D, KV_HEADS * HEAD_DIM), D ** -0.5, 0.125, ((1, 8), (2, 4)))
    output_weight = bell_draw(streams_of[5], (LAYERS, D, HEADS * HEAD_DIM), (HEADS * HEAD_DIM) ** -0.5, 0.1875, ((1, 8), (2, 4)))
    sink_logit = jnp.clip(2.0 + 5.0 * jax.random.uniform(streams_of[6], (LAYERS, HEADS), jnp.float32) ** level_of(streams_of[6], (LAYERS, HEADS), ((1, 4),), -0.2, 0.2), 2.0, 7.0)
    final_gain = jnp.clip(1.0 + 0.18 * jax.random.normal(streams_of[7], (D,), jnp.float32), 0.1, 1.9)
    return {"inputs": inputs, "norm_gain": norm_gain, "query_weight": query_weight, "key_weight": key_weight, "value_weight": value_weight, "output_weight": output_weight, "sink_logit": sink_logit, "final_gain": final_gain}


EPS = 1e-06

def norm_rows(values, gain):
    wide_values = values.astype(jnp.float32)
    inv_root = lax.rsqrt(lax.optimization_barrier(jnp.mean(wide_values * wide_values, axis=-1, keepdims=True)) + EPS)
    return wide_values * inv_root * gain

def rotate(values, places):
    half_dim = values.shape[-1] // 2
    inverse = 10000.0 ** (-jnp.arange(half_dim).astype(jnp.float32) / half_dim)
    angles = places[:, None] * inverse[None, :]
    cosine_table = jnp.cos(angles)[:, None, :]
    sine_table = jnp.sin(angles)[:, None, :]
    front_half = values[..., :half_dim]
    back_half = values[..., half_dim:]
    return jnp.concatenate([front_half * cosine_table - back_half * sine_table, back_half * cosine_table + front_half * sine_table], axis=-1)

def attend(queries, key_rows, value_rows, sink_row, allowed):
    scores = jnp.einsum('qkgd,skd->kgqs', queries.astype(jnp.float32), key_rows.astype(jnp.float32)) * queries.shape[-1] ** (-0.5)
    scores = jnp.where(allowed[None, None], scores, -jnp.inf)
    sink_col = sink_row[:, :, None]
    largest = jnp.maximum(lax.optimization_barrier(jnp.max(scores, axis=-1)), sink_col)
    powers = jnp.exp(scores - largest[..., None])
    denominator = lax.optimization_barrier(jnp.sum(powers, axis=-1)) + jnp.exp(sink_col - largest)
    weights = (powers / denominator[..., None]).astype(jnp.bfloat16)
    blended = jnp.einsum('kgqs,skd->qkgd', weights.astype(jnp.float32), value_rows.astype(jnp.float32))
    return blended.astype(jnp.bfloat16)

def reference(inputs, norm_gain, query_weight, key_weight, value_weight, output_weight, sink_logit, final_gain):
    seq_total = inputs.shape[0]
    blocks = seq_total // TOK_DEV
    per_group = HEADS // KV_HEADS
    places = jnp.arange(seq_total).astype(jnp.float32)
    current = inputs
    for layer in range(LAYERS):
        normed = norm_rows(current, norm_gain[layer]).astype(jnp.bfloat16)
        query_raw = jnp.dot(normed, query_weight[layer], preferred_element_type=jnp.float32) * float(D) ** (-0.5)
        key_raw = jnp.dot(normed, key_weight[layer], preferred_element_type=jnp.float32) * float(D) ** (-0.5)
        value_raw = jnp.dot(normed, value_weight[layer], preferred_element_type=jnp.float32)
        queries = rotate(query_raw.reshape(seq_total, HEADS, HEAD_DIM), places).astype(jnp.bfloat16)
        queries = queries.reshape(seq_total, KV_HEADS, per_group, HEAD_DIM)
        key_rot = rotate(key_raw.reshape(seq_total, KV_HEADS, HEAD_DIM), places).astype(jnp.bfloat16)
        value_all = value_raw.astype(jnp.bfloat16).reshape(seq_total, KV_HEADS, HEAD_DIM)
        padding = ((WINDOW, WINDOW), (0, 0), (0, 0))
        pad_keys = jnp.pad(key_rot, padding)
        pad_values = jnp.pad(value_all, padding)
        sink_row = sink_logit[layer].reshape(KV_HEADS, per_group)

        def one_block(block_index):
            first_row = block_index * TOK_DEV
            block_queries = lax.dynamic_slice_in_dim(queries, first_row, TOK_DEV, 0)
            block_keys = lax.dynamic_slice_in_dim(pad_keys, first_row, TOK_DEV + 2 * WINDOW, 0)
            block_values = lax.dynamic_slice_in_dim(pad_values, first_row, TOK_DEV + 2 * WINDOW, 0)
            query_pos = first_row + jnp.arange(TOK_DEV, dtype=jnp.int32)
            key_pos = first_row - WINDOW + jnp.arange(TOK_DEV + 2 * WINDOW, dtype=jnp.int32)
            allowed = (jnp.abs(key_pos[None, :] - query_pos[:, None]) <= WINDOW) & (key_pos[None, :] >= 0) & (key_pos[None, :] < seq_total)
            return attend(block_queries, block_keys, block_values, sink_row, allowed)
        attended = lax.map(one_block, jnp.arange(blocks, dtype=jnp.int32)).reshape(seq_total, HEADS * HEAD_DIM)
        current = jnp.dot(attended, output_weight[layer].T, preferred_element_type=jnp.float32).astype(jnp.bfloat16)
    return norm_rows(current, final_gain)
```

```python
import functools
import math

import jax
import jax.numpy as jnp
from jax import lax
from jax.experimental import pallas as pl
from jax.experimental.pallas import tpu as pltpu
from jax.sharding import PartitionSpec as P

HEAD_DIM = 64
WINDOW = 128
EPS = 1e-06
LANES = 128
F32 = jnp.float32
BF16 = jnp.bfloat16
VMEM_LIMIT = 60 * 1024 * 1024
KINDS = 3
SPLIT = 2
AHEAD = 3
WHOLE = slice(None)


def grid_of(mesh):
    n_sp, n_tp = mesh.shape["sp"], mesh.shape["tp"]
    devices = mesh.devices
    n_z = len({d.coords[2] for d in devices[:, 0]})
    n_x = len({d.coords[0] for d in devices[0, :]})
    return n_z, n_sp // n_z, n_x, n_tp // n_x


def stack_kernel(grid, sources, *refs):
    n_z, n_y, n_x, n_c = grid
    n_sp, n_tp = n_z * n_y, n_x * n_c
    (inputs_ref, gain_ref, last_gain_ref, sink_ref, trig_ref), refs = refs[:5], refs[5:]
    weight_refs, refs = refs[: len(sources)], refs[len(sources) :]
    out_ref, refs = refs[0], refs[1:]
    w, state, normed, queries, kv, attended, bias, tables, sinks = refs[:9]
    send_sem, recv_sem, halo_send, halo_recv, sink_send, sink_recv, local_sem = refs[9:]

    layers, rows, cols = w.shape[1], w.shape[6], w.shape[7]
    tokens, features = state.shape
    heads = cols // HEAD_DIM
    groups = heads // 2
    kv_cols = cols // 2
    per_group = heads // groups
    blocks = tokens // WINDOW

    sp, tp = lax.axis_index("sp"), lax.axis_index("tp")
    place = sp * n_tp + tp
    z, y, x, core = sp // n_y, sp % n_y, tp // n_c, tp % n_c
    at = {"z": z, "y": y, "x": x}
    size = {"z": n_z, "y": n_y, "x": n_x}
    other = 1 - core

    def device(**where):
        to = dict(at, core=core)
        to.update(where)
        return {"sp": to["z"] * n_y + to["y"], "tp": to["x"] * n_c + to["core"]}

    def linear(index):
        return {"sp": index // n_tp, "tp": index % n_tp}

    half = rows // SPLIT
    units = [(layer, kind, piece) for layer in range(layers) for kind in range(KINDS) for piece in range(SPLIT)]

    def order_of(colour, u):
        first, second = ("y", "x") if colour == 0 else ("x", "y")
        return ("z", first, second) if u % 3 != 2 else (first, "z", second)

    def block(u, colour, **where):
        layer, kind, piece = units[u]
        spot = dict({"z": z, "y": y, "x": x}, **where)
        return w.at[kind, layer, spot["x"], colour, spot["z"], spot["y"], pl.ds(piece * half, half)]

    most = max(size.values())
    hops = 3 * (most - 1)
    per_unit = hops + most

    def remote(src, dst, number, to):
        return pltpu.make_async_remote_copy(
            src_ref=src, dst_ref=dst, send_sem=send_sem.at[number], recv_sem=recv_sem.at[number],
            device_id=to, device_id_type=pl.DeviceIdType.MESH,
        )

    def staged(u, colour, stage, k, arriving):
        order = order_of(colour, u)
        axis = order[stage]
        spot = {a: WHOLE for a in order[:stage]}
        if arriving:
            spot[axis] = (at[axis] + size[axis] - k) % size[axis]
        view = block(u, colour, **spot)
        to = device(**{axis: (at[axis] + k) % size[axis]})
        return remote(view, view, u * per_unit + stage * (most - 1) + k - 1, to)

    def shared(u, colour, k):
        order = order_of(colour, u)
        spot = {a: WHOLE for a in order[:2]}
        axis = order[2]
        spot[axis] = (at[axis] + size[axis] - k) % size[axis]
        view = block(u, colour, **spot)
        return remote(view, view, u * per_unit + hops + k, device(core=other))

    def by_core(do):
        for colour in range(n_c):
            pl.when(core == colour)(functools.partial(do, colour))

    def send_stage(u, stage):
        def do(colour):
            for k in range(1, size[order_of(colour, u)[stage]]):
                staged(u, colour, stage, k, False).start()
        by_core(do)

    def wait_stage(u, stage):
        def do(colour):
            for k in range(1, size[order_of(colour, u)[stage]]):
                staged(u, colour, stage, k, True).wait_recv()
        by_core(do)

    def share(u, first):
        def do(colour):
            last = size[order_of(colour, u)[2]]
            for k in range(1) if first else range(1, last):
                shared(u, colour, k).start()
        by_core(do)

    def wait_shared(u):
        def do(colour):
            for k in range(size[order_of(1 - colour, u)[2]]):
                shared(u, 1 - colour, k).wait_recv()
        by_core(do)

    def drain(u):
        def do(colour):
            for stage in range(3):
                for k in range(1, size[order_of(colour, u)[stage]]):
                    staged(u, colour, stage, k, False).wait_send()
            for k in range(size[order_of(colour, u)[2]]):
                shared(u, colour, k).wait_send()
        by_core(do)

    own = []
    for i, (kind, offset, width) in enumerate(sources):
        dst = w.at[kind, :, x, core, z, y, :, pl.ds(offset, width)]
        own.append(pltpu.make_async_copy(weight_refs[i], dst, local_sem.at[i]))
    own.append(
        pltpu.make_async_copy(
            inputs_ref.at[pl.ds(pl.multiple_of(tp * tokens, tokens), tokens)], state, local_sem.at[len(sources)]
        )
    )
    for copy in own:
        copy.start()

    barrier = pltpu.get_barrier_semaphore()

    def greet(to):
        pl.semaphore_signal(barrier, inc=1, device_id=to, device_id_type=pl.DeviceIdType.MESH)

    met = 0
    for axis in ("z", "y", "x"):
        for k in range(1, size[axis]):
            greet(device(**{axis: (at[axis] + k) % size[axis]}))
            met += 1
    for k in range(1, n_tp):
        greet({"sp": sp, "tp": (tp + k) % n_tp})
        met += 1
    has_low, has_high = place > 0, place < n_sp * n_tp - 1
    everyone = n_sp * n_tp
    greet(linear((place + 1) % everyone))
    greet(linear((place + everyone - 1) % everyone))
    for copy in own[:-1]:
        copy.wait()
    pl.semaphore_wait(barrier, met + 2)

    for u in range(AHEAD):
        send_stage(u, 0)

    def sink_copy(k, arriving):
        source = (tp + n_tp - k) % n_tp if arriving else tp
        return pltpu.make_async_remote_copy(
            src_ref=sink_ref, dst_ref=sinks.at[source], send_sem=sink_send.at[k - 1], recv_sem=sink_recv.at[k - 1],
            device_id={"sp": sp, "tp": (tp + k) % n_tp}, device_id_type=pl.DeviceIdType.MESH,
        )

    for k in range(1, n_tp):
        sink_copy(k, False).start()
    sinks[tp] = sink_ref[...]

    pair_c, pair_s = trig_ref[:, :HEAD_DIM], trig_ref[:, HEAD_DIM:]
    root = HEAD_DIM ** (-0.5)
    one = jnp.ones((tokens, kv_cols), F32)
    tables[0] = jnp.concatenate([pair_c] * groups + [one], axis=1)
    tables[1] = jnp.concatenate([pair_s] * groups + [0 * one], axis=1)
    tables[2] = jnp.concatenate([pair_c * root] * heads, axis=1)
    tables[3] = jnp.concatenate([pair_s * root] * heads, axis=1)
    span = 3 * WINDOW
    row = lax.broadcasted_iota(jnp.int32, (WINDOW, span), 0)
    reach = lax.broadcasted_iota(jnp.int32, (WINDOW, span), 1) - WINDOW
    for b in range(blocks):
        key_pos = place * tokens + b * WINDOW + reach
        allowed = (jnp.abs(row - reach) <= WINDOW) & (key_pos >= 0) & (key_pos < n_sp * n_tp * tokens)
        bias[b] = jnp.where(allowed, 0.0, -jnp.inf).astype(F32)

    nothing = jnp.zeros((layers, n_tp, WINDOW, cols), BF16)

    @pl.when(jnp.logical_not(has_low))
    def _():
        kv[:, :, :WINDOW] = nothing

    @pl.when(jnp.logical_not(has_high))
    def _():
        kv[:, :, WINDOW + tokens :] = nothing

    def halo(layer, t, up):
        here = pl.ds(tokens, WINDOW) if up else pl.ds(WINDOW, WINDOW)
        there = pl.ds(0, WINDOW) if up else pl.ds(WINDOW + tokens, WINDOW)
        number = (layer * n_tp + t) * 2 + int(up)
        return pltpu.make_async_remote_copy(
            src_ref=kv.at[layer, t, here], dst_ref=kv.at[layer, t, there],
            send_sem=halo_send.at[number], recv_sem=halo_recv.at[number],
            device_id=linear(place + 1 if up else place - 1), device_id_type=pl.DeviceIdType.MESH,
        )

    def norm(layer):
        if layer == 0:
            own[-1].wait()
        wide = state[...].astype(F32)
        inv_root = lax.rsqrt(jnp.mean(wide * wide, axis=-1, keepdims=True) + EPS)
        normed[...] = (wide * inv_root * gain_ref[layer : layer + 1]).astype(BF16)

    lane = lax.broadcasted_iota(jnp.int32, (tokens, cols), 1)
    front = (lane % HEAD_DIM) < HEAD_DIM // 2

    def project(layer, kind, t):
        weight = w[kind, layer, t // n_c, t % n_c].reshape(features, cols)
        acc = jnp.dot(normed[...], weight, preferred_element_type=F32)
        step = HEAD_DIM // 2
        partner = jnp.where(front, pltpu.roll(acc, cols - step, 1), pltpu.roll(acc, step, 1))
        return (acc * tables[2 * kind] + partner * tables[2 * kind + 1]).astype(BF16)

    def make_kv(layer, t):
        kv[layer, t, WINDOW : WINDOW + tokens] = project(layer, 0, t)

    def make_q(layer, t):
        queries[t] = project(layer, 1, t)

    def send_halo(layer, t):
        pl.when(has_low)(lambda: halo(layer, t, False).start())
        pl.when(has_high)(lambda: halo(layer, t, True).start())

    row_head = lax.broadcasted_iota(jnp.int32, (per_group * WINDOW, 1), 0) // WINDOW

    def attend(layer, t, b):
        if b == 0:
            pl.when(has_low)(lambda: halo(layer, t, True).wait_recv())
        if b == blocks - 1:
            pl.when(has_high)(lambda: halo(layer, t, False).wait_recv())
        here = slice(b * WINDOW, (b + 1) * WINDOW)
        near = slice(b * WINDOW, b * WINDOW + span)
        near_bias = jnp.concatenate([bias[b]] * per_group, axis=0)
        for g in range(groups):
            first = g * per_group
            k = kv[layer, t, near, g * HEAD_DIM : (g + 1) * HEAD_DIM]
            v = kv[layer, t, near, kv_cols + g * HEAD_DIM : kv_cols + (g + 1) * HEAD_DIM]
            q = jnp.concatenate(
                [queries[t, here, h * HEAD_DIM : (h + 1) * HEAD_DIM] for h in range(first, first + per_group)], axis=0
            )
            scores = lax.dot_general(q, k, (((1,), (1,)), ((), ())), preferred_element_type=F32) + near_bias
            sink = jnp.zeros((per_group * WINDOW, 1), F32)
            for e in range(per_group):
                sink = jnp.where(row_head == e, sinks[t, layer : layer + 1, first + e : first + e + 1], sink)
            largest = jnp.maximum(jnp.max(scores, axis=-1, keepdims=True), sink)
            powers = jnp.exp(scores - largest)
            total = jnp.sum(powers, axis=-1, keepdims=True) + jnp.exp(sink - largest)
            mixed = jnp.dot(powers.astype(BF16), v, preferred_element_type=F32) * (1.0 / total)
            mixed = mixed.astype(BF16)
            attended[t, here, first * HEAD_DIM : (first + per_group) * HEAD_DIM] = jnp.concatenate(
                [mixed[e * WINDOW : (e + 1) * WINDOW] for e in range(per_group)], axis=1
            )

    def make_state(layer, s):
        piece = jnp.zeros((tokens, rows), F32)
        for t in range(n_tp):
            piece += lax.dot_general(
                attended[t], w[2, layer, t // n_c, t % n_c, s // n_y, s % n_y],
                (((1,), (1,)), ((), ())), preferred_element_type=F32,
            )
        state[:, s * rows : (s + 1) * rows] = piece.astype(BF16)

    def finish():
        wide = state[...].astype(F32)
        inv_root = lax.rsqrt(jnp.mean(wide * wide, axis=-1, keepdims=True) + EPS)
        out_ref[...] = wide * inv_root * last_gain_ref[...]

    work = []
    for layer in range(layers):
        arrived = [(layer * KINDS + kind + 1) * SPLIT - 1 for kind in range(KINDS)]
        work.append((-1 if layer == 0 else arrived[0] - 1, 1.0, functools.partial(norm, layer)))
        for t in range(n_tp):
            work.append((arrived[0], 0.8, functools.partial(make_kv, layer, t)))
            if t:
                work.append((arrived[0], 0.0, functools.partial(send_halo, layer, t - 1)))
        for t in range(n_tp):
            work.append((arrived[1], 0.8, functools.partial(make_q, layer, t)))
            if t == 0:
                work.append((arrived[1], 0.0, functools.partial(send_halo, layer, n_tp - 1)))
        if layer == 0:
            def sinks_here():
                for k in range(1, n_tp):
                    sink_copy(k, True).wait_recv()
            work.append((arrived[1], 0.0, sinks_here))
        for t in range(n_tp):
            for b in range(blocks):
                work.append((arrived[1], 0.6, functools.partial(attend, layer, t, b)))
        for s in range(n_sp):
            work.append((arrived[2], 0.4, functools.partial(make_state, layer, s)))
    work.append((len(units) - 1, 1.0, finish))

    done = -1

    def compute(budget):
        while work and work[0][0] <= done and budget > 0:
            _, cost, piece = work.pop(0)
            piece()
            budget -= cost

    compute(9.0)
    count = len(units)
    for s in range(count + 3):
        if AHEAD <= s + AHEAD < count:
            send_stage(s + AHEAD, 0)
        if s < count:
            wait_stage(s, 0)
            send_stage(s, 1)
        compute(1.5)
        if 0 <= s - 1 < count:
            wait_stage(s - 1, 1)
            send_stage(s - 1, 2)
            share(s - 1, True)
        compute(1.5)
        if 0 <= s - 2 < count:
            wait_stage(s - 2, 2)
            share(s - 2, False)
        compute(1.5)
        if 0 <= s - 3 < count:
            wait_shared(s - 3)
            done = s - 3
        compute(1.5)
    compute(math.inf)

    for u in range(count):
        drain(u)
    for k in range(1, n_tp):
        sink_copy(k, False).wait_send()
    for layer in range(layers):
        for t in range(n_tp):
            pl.when(has_low)(lambda: halo(layer, t, False).wait_send())
            pl.when(has_high)(lambda: halo(layer, t, True).wait_send())


def shards(
    grid, inputs, norm_gain, query_weight, key_weight, value_weight, output_weight, sink_logit, final_gain
):
    n_z, n_y, n_x, n_c = grid
    n_sp, n_tp = n_z * n_y, n_x * n_c
    layers, rows, cols = query_weight.shape
    kv_cols = key_weight.shape[2]
    features = inputs.shape[1]
    tokens = inputs.shape[0] // n_tp
    place = lax.axis_index("sp") * n_tp + lax.axis_index("tp")

    half = HEAD_DIM // 2
    inverse = 10000.0 ** (-jnp.arange(half).astype(F32) / half)
    places = (place * tokens + jnp.arange(tokens, dtype=jnp.int32)).astype(F32)
    angles = places[:, None] * inverse[None, :]
    cosine, sine = jnp.cos(angles), jnp.sin(angles)
    scale = float(features) ** (-0.5)
    trig = jnp.concatenate([cosine, cosine, -sine, sine], axis=1) * scale

    if kv_cols % LANES:
        weights = [jnp.concatenate([key_weight, value_weight], axis=2), query_weight, output_weight]
        sources = [(0, 0, cols), (1, 0, cols), (2, 0, cols)]
    else:
        weights = [key_weight, value_weight, query_weight, output_weight]
        sources = [(0, 0, kv_cols), (0, kv_cols, kv_cols), (1, 0, cols), (2, 0, cols)]

    most = max(n_z, n_y, n_x)
    copies = layers * KINDS * SPLIT * (3 * (most - 1) + most)
    vmem = pl.BlockSpec(memory_space=pltpu.VMEM)
    hbm = pl.BlockSpec(memory_space=pl.ANY)
    return pl.pallas_call(
        functools.partial(stack_kernel, grid, sources),
        name="stack",
        out_shape=jax.ShapeDtypeStruct((tokens, features), F32),
        in_specs=[hbm, vmem, vmem, vmem, vmem] + [hbm] * len(weights),
        out_specs=vmem,
        scratch_shapes=[
            pltpu.VMEM((KINDS, layers, n_x, n_c, n_z, n_y, rows, cols), BF16),
            pltpu.VMEM((tokens, features), BF16),
            pltpu.VMEM((tokens, features), BF16),
            pltpu.VMEM((n_tp, tokens, cols), BF16),
            pltpu.VMEM((layers, n_tp, tokens + 2 * WINDOW, cols), BF16),
            pltpu.VMEM((n_tp, tokens, cols), BF16),
            pltpu.VMEM((tokens // WINDOW, WINDOW, 3 * WINDOW), F32),
            pltpu.VMEM((4, tokens, cols), F32),
            pltpu.VMEM((n_tp,) + sink_logit.shape, F32),
            pltpu.SemaphoreType.DMA((copies,)),
            pltpu.SemaphoreType.DMA((copies,)),
            pltpu.SemaphoreType.DMA((layers * n_tp * 2,)),
            pltpu.SemaphoreType.DMA((layers * n_tp * 2,)),
            pltpu.SemaphoreType.DMA((n_tp - 1,)),
            pltpu.SemaphoreType.DMA((n_tp - 1,)),
            pltpu.SemaphoreType.DMA((len(weights) + 1,)),
        ],
        compiler_params=pltpu.CompilerParams(
            vmem_limit_bytes=VMEM_LIMIT, collective_id=0, has_side_effects=True
        ),
    )(inputs, norm_gain, final_gain[None], sink_logit, trig, *weights)


def solution(mesh):
    in_specs = (
        P("sp", None),
        P(),
        P(None, "sp", "tp"),
        P(None, "sp", "tp"),
        P(None, "sp", "tp"),
        P(None, "sp", "tp"),
        P(None, "tp"),
        P(),
    )
    out_specs = P(("sp", "tp"), None)
    return jax.shard_map(
        functools.partial(shards, grid_of(mesh)), mesh=mesh, in_specs=in_specs, out_specs=out_specs, check_vma=False
    )
```

```python
import functools
import math

import jax
import jax.numpy as jnp
from jax import lax
from jax.experimental import pallas as pl
from jax.experimental.pallas import tpu as pltpu
from jax.sharding import PartitionSpec as P

HEAD_DIM = 64
WINDOW = 128
EPS = 1e-06
LANES = 128
F32 = jnp.float32
BF16 = jnp.bfloat16
VMEM_LIMIT = 60 * 1024 * 1024
KINDS = 3
SPLIT = 4
AHEAD = 2
LAGS = (0, 1, 2, 3, 4, 5)
SLOTS = (0, 1, 0, 1)
LATE = (1, 1, 1, 1)
LATE_FROM = 0.75
SETTLE = 4
WHOLE = slice(None)
LINE = 4


def grid_of(mesh):
    n_sp, n_tp = mesh.shape["sp"], mesh.shape["tp"]
    devices = mesh.devices
    n_z = len({d.coords[2] for d in devices[:, 0]})
    n_x = len({d.coords[0] for d in devices[0, :]})
    return n_z, n_sp // n_z, n_x, n_tp // n_x


def unit_list(layers, rows):
    units = []
    n = 0
    for layer in range(layers):
        for kind in range(KINDS):
            for piece in range(SPLIT):
                size = rows // SPLIT
                if layer == 0 and kind < 2:
                    orders = (("z", "y"), ("z", "y"))
                else:
                    orders = FLAVOURS[PATTERN[n % len(PATTERN)]]
                    n += 1
                units.append((layer, kind, piece * size, size, orders))
    return units


FLAVOURS = {
    "a": (("z", "y", "x"), ("z", "x", "y")),
    "b": (("y", "z", "x"), ("x", "z", "y")),
    "A": (("z", "y", "x"), ("z", "y", "x")),
    "B": (("y", "z", "x"), ("y", "z", "x")),
    "c": (("y", "x", "z"), ("x", "y", "z")),
    "e": (("z", "y", "x"), ("x", "z", "y")),
    "f": (("y", "z", "x"), ("z", "x", "y")),
}
PATTERN = "Abbabbabbabbab"


def normalize(wide, gain):
    inv_root = lax.rsqrt(jnp.mean(wide * wide, axis=-1, keepdims=True) + EPS)
    return wide * inv_root * gain


def finish_kernel(state_ref, gain_ref, out_ref):
    out_ref[...] = normalize(state_ref[...].astype(F32), gain_ref[...])


def stack_kernel(grid, sources, units, *refs):
    n_z, n_y, n_x, n_c = grid
    n_sp, n_tp = n_z * n_y, n_x * n_c
    (inputs_ref, gain_ref, sink_ref, inverse_ref), refs = refs[:4], refs[4:]
    weight_refs, refs = refs[: len(sources)], refs[len(sources) :]
    out_ref, refs = refs[0], refs[1:]
    w, stage_in, state, normed, queries, kv0, kv, mine, attended, bias, trig, tables, sinks = refs[:13]
    send_sem, recv_sem, halo_send, halo_recv, slice_send, slice_recv, sink_send, sink_recv, local_sem = refs[13:]

    layers, rows, cols = w.shape[1], w.shape[6], w.shape[7]
    tokens, features = state.shape
    span = n_tp * tokens
    heads = cols // HEAD_DIM
    groups = heads // 2
    kv_cols = cols // 2
    per_group = heads // groups
    blocks = tokens // WINDOW

    sp, tp = lax.axis_index("sp"), lax.axis_index("tp")
    place = sp * n_tp + tp
    z, y, x, core = sp // n_y, sp % n_y, tp // n_c, tp % n_c
    at = {"z": z, "y": y, "x": x}
    size = {"z": n_z, "y": n_y, "x": n_x}
    other = 1 - core

    def device(**where):
        to = dict(at, core=core)
        to.update(where)
        return {"sp": to["z"] * n_y + to["y"], "tp": to["x"] * n_c + to["core"]}

    def linear(index):
        return {"sp": index // n_tp, "tp": index % n_tp}

    def send(src, dst, send_at, recv_at, to):
        return pltpu.make_async_remote_copy(
            src_ref=src, dst_ref=dst, send_sem=send_at, recv_sem=recv_at,
            device_id=to, device_id_type=pl.DeviceIdType.MESH,
        )

    base = {"z": 0, "y": n_z - 1, "x": n_z + n_y - 2}
    hops = n_z + n_y + n_x - 3
    per_unit = hops + 1 + max(size.values())

    def relayed(axis):
        return axis == "z" and size[axis] == LINE

    def block(u, colour, **where):
        layer, kind, first, count, _ = units[u]
        spot = dict({"z": z, "y": y, "x": x}, **where)
        return w.at[kind, layer, spot["x"], colour, spot["z"], spot["y"], pl.ds(first, count)]

    def part(u, colour, stage, source):
        order = units[u][4][colour]
        spot = {a: WHOLE for a in order[:stage]}
        spot[order[stage]] = source
        return block(u, colour, **spot)

    def staged(u, colour, stage, k, arriving):
        axis = units[u][4][colour][stage]
        view = part(u, colour, stage, (at[axis] + size[axis] - k) % size[axis] if arriving else at[axis])
        number = u * per_unit + base[axis] + k - 1
        to = device(**{axis: (at[axis] + k) % size[axis]})
        return send(view, view, send_sem.at[number], recv_sem.at[number], to)

    def relay(u, colour, stage, inner):
        source, target = (LINE - 1, 0) if inner == 1 else (0, LINE - 1)
        view = part(u, colour, stage, source)
        number = u * per_unit
        k = (target - source) % LINE
        return send(view, view, send_sem.at[number + hops], recv_sem.at[number + k - 1], device(z=target))

    def shared(u, colour, k):
        axis = units[u][4][colour][2]
        view = part(u, colour, 2, (at[axis] + size[axis] - k) % size[axis])
        number = u * per_unit + hops + 1 + k
        return send(view, view, send_sem.at[number], recv_sem.at[number], device(core=other))

    def outgoing(u, colour, stage, do):
        axis = units[u][4][colour][stage]
        if relayed(axis):
            do(staged(u, colour, stage, 2, False))
            pl.when(z != LINE - 1)(lambda: do(staged(u, colour, stage, 1, False)))
            pl.when(z != 0)(lambda: do(staged(u, colour, stage, 3, False)))
        else:
            for k in range(1, size[axis]):
                do(staged(u, colour, stage, k, False))

    def by_core(do):
        for colour in range(n_c):
            pl.when(core == colour)(functools.partial(do, colour))

    def depart(u):
        by_core(lambda colour: outgoing(u, colour, 0, lambda c: c.start()))

    def pass_on(u, stage):
        def do(colour):
            order = units[u][4][colour]
            if stage < len(order) and relayed(order[stage]):
                staged(u, colour, stage, 2, True).wait_recv()
                for inner in (1, 2):
                    pl.when(z == inner)(lambda: relay(u, colour, stage, inner).start())
        by_core(do)

    def advance(u, stage):
        def do(colour):
            order = units[u][4][colour]
            if stage >= len(order):
                return
            axis = order[stage]
            for k in range(1, size[axis]):
                if not (relayed(axis) and k == 2):
                    staged(u, colour, stage, k, True).wait_recv()
            if stage + 1 < len(order):
                outgoing(u, colour, stage + 1, lambda c: c.start())
            if stage == 1 and len(order) == 3:
                shared(u, colour, 0).start()
            if stage == 2:
                for k in range(1, size[axis]):
                    shared(u, colour, k).start()
        by_core(do)

    def wait_shared(u):
        def do(colour):
            order = units[u][4][1 - colour]
            if len(order) == 3:
                for k in range(size[order[2]]):
                    shared(u, 1 - colour, k).wait_recv()
        by_core(do)

    def drain(u):
        def do(colour):
            order = units[u][4][colour]
            for stage, axis in enumerate(order):
                outgoing(u, colour, stage, lambda c: c.wait_send())
                if relayed(axis):
                    for inner in (1, 2):
                        pl.when(z == inner)(lambda: relay(u, colour, stage, inner).wait_send())
            if len(order) == 3:
                for k in range(size[order[2]]):
                    shared(u, colour, k).wait_send()
        by_core(do)

    own = []
    for i, (kind, offset, width) in enumerate(sources):
        dst = w.at[kind, :, x, core, z, y, :, pl.ds(offset, width)]
        own.append(pltpu.make_async_copy(weight_refs[i], dst, local_sem.at[i]))
    for copy in own:
        copy.start()

    def fetch(i):
        return pltpu.make_async_copy(
            inputs_ref.at[pl.ds(i * tokens, tokens)], stage_in.at[i % 2], local_sem.at[len(sources) + i]
        )

    for i in range(2):
        fetch(i).start()

    barrier = pltpu.get_barrier_semaphore()

    def greet(to):
        pl.semaphore_signal(barrier, inc=1, device_id=to, device_id_type=pl.DeviceIdType.MESH)

    everyone = n_sp * n_tp
    met = [device(**{axis: (at[axis] + k) % size[axis]}) for axis in ("z", "y", "x") for k in range(1, size[axis])]
    met += [{"sp": sp, "tp": (tp + k) % n_tp} for k in range(1, n_tp)]
    met += [linear((place + step) % everyone) for step in (1, everyone - 1)]
    met += [{"sp": (sp + step) % n_sp, "tp": tp} for step in (1, n_sp - 1)]
    for to in met:
        greet(to)
    for copy in own:
        copy.wait()
    pl.semaphore_wait(barrier, len(met))

    count = len(units)
    for u in range(AHEAD):
        depart(u)

    def sink_copy(k, arriving):
        source = (tp + n_tp - k) % n_tp if arriving else tp
        to = {"sp": sp, "tp": (tp + k) % n_tp}
        return send(sink_ref, sinks.at[source], sink_send.at[k - 1], sink_recv.at[k - 1], to)

    for k in range(1, n_tp):
        sink_copy(k, False).start()
    sinks[tp] = sink_ref[...]

    root = HEAD_DIM ** (-0.5)
    scale = float(features) ** (-0.5)

    def fill(i, carry):
        first = sp * span + i * WINDOW
        where = lax.broadcasted_iota(jnp.int32, (WINDOW, 2 * HEAD_DIM), 0) + first
        angles = where.astype(F32) * inverse_ref[...]
        column = lax.broadcasted_iota(jnp.int32, (WINDOW, 2 * HEAD_DIM), 1)
        sine = jnp.sin(angles)
        turned = jnp.where(column < HEAD_DIM + HEAD_DIM // 2, -sine, sine)
        trig[pl.ds(pl.multiple_of(i * WINDOW, WINDOW), WINDOW)] = (
            jnp.where(column < HEAD_DIM, jnp.cos(angles), turned) * scale
        )
        return carry

    lax.fori_loop(0, span // WINDOW, fill, 0)

    def turn_tables(kind, where):
        pair_c, pair_s = trig[where, :HEAD_DIM], trig[where, HEAD_DIM:]
        if kind:
            return jnp.concatenate([pair_c * root] * heads, axis=1), jnp.concatenate([pair_s * root] * heads, axis=1)
        one = jnp.ones((tokens, kv_cols), F32)
        return jnp.concatenate([pair_c] * groups + [one], axis=1), jnp.concatenate([pair_s] * groups + [0 * one], axis=1)

    for kind in range(2):
        tables[2 * kind], tables[2 * kind + 1] = turn_tables(kind, pl.ds(pl.multiple_of(tp * tokens, tokens), tokens))
    reach_of = 3 * WINDOW
    row = lax.broadcasted_iota(jnp.int32, (WINDOW, reach_of), 0)
    reach = lax.broadcasted_iota(jnp.int32, (WINDOW, reach_of), 1) - WINDOW
    for b in range(span // WINDOW):
        key_pos = sp * span + b * WINDOW + reach
        allowed = (jnp.abs(row - reach) <= WINDOW) & (key_pos >= 0) & (key_pos < n_sp * span)
        bias[b] = jnp.where(allowed, 0.0, -jnp.inf).astype(F32)

    has_low, has_high = place > 0, place < everyone - 1
    span_low, span_high = sp > 0, sp < n_sp - 1
    nothing = jnp.zeros((layers - 1, n_tp, WINDOW, cols), BF16)

    @pl.when(jnp.logical_not(has_low))
    def _():
        kv[:, :, :WINDOW] = nothing

    @pl.when(jnp.logical_not(has_high))
    def _():
        kv[:, :, WINDOW + tokens :] = nothing

    @pl.when(jnp.logical_not(span_low))
    def _():
        kv0[:WINDOW] = nothing[0, 0]

    @pl.when(jnp.logical_not(span_high))
    def _():
        kv0[WINDOW + span :] = nothing[0, 0]

    def halo(layer, t, up):
        length = span if layer == 0 else tokens
        here = pl.ds(length, WINDOW) if up else pl.ds(WINDOW, WINDOW)
        there = pl.ds(0, WINDOW) if up else pl.ds(WINDOW + length, WINDOW)
        number = (layer * n_tp + t) * 2 + int(up)
        rows_of = kv0 if layer == 0 else kv.at[layer - 1, t]
        step = 1 if up else -1
        to = {"sp": sp + step, "tp": tp} if layer == 0 else linear(place + step)
        return send(rows_of.at[here], rows_of.at[there], halo_send.at[number], halo_recv.at[number], to)

    def low_high(layer):
        return (span_low, span_high) if layer == 0 else (has_low, has_high)

    def send_halo(layer, t):
        low, high = low_high(layer)
        pl.when(low)(lambda: halo(layer, t, False).start())
        pl.when(high)(lambda: halo(layer, t, True).start())

    def wait_halo(layer, t):
        low, high = low_high(layer)
        pl.when(low)(lambda: halo(layer, t, True).wait_recv())
        pl.when(high)(lambda: halo(layer, t, False).wait_recv())

    def norm0(i):
        fetch(i).wait()
        normed[i] = normalize(stage_in[i % 2].astype(F32), gain_ref[0:1]).astype(BF16)
        if i + 2 < n_tp:
            fetch(i + 2).start()

    def norm(layer):
        normed[0] = normalize(state[...].astype(F32), gain_ref[layer : layer + 1]).astype(BF16)

    lane = lax.broadcasted_iota(jnp.int32, (tokens, cols), 1)
    front = (lane % HEAD_DIM) < HEAD_DIM // 2

    def project(chunk, weight, cos_table, sin_table):
        acc = jnp.dot(normed[chunk], weight.reshape(features, cols), preferred_element_type=F32)
        step = HEAD_DIM // 2
        partner = jnp.where(front, pltpu.roll(acc, cols - step, 1), pltpu.roll(acc, step, 1))
        return (acc * cos_table + partner * sin_table).astype(BF16)

    def make_kv0(i):
        kv0[WINDOW + i * tokens : WINDOW + (i + 1) * tokens] = project(
            i, w[0, 0, x, core], *turn_tables(0, pl.ds(i * tokens, tokens))
        )

    def make_q0(i):
        queries[i] = project(i, w[1, 0, x, core], *turn_tables(1, pl.ds(i * tokens, tokens)))

    def make_kv(layer, t):
        kv[layer - 1, t, WINDOW : WINDOW + tokens] = project(0, w[0, layer, t // n_c, t % n_c], tables[0], tables[1])

    def make_q(layer, t):
        queries[t] = project(0, w[1, layer, t // n_c, t % n_c], tables[2], tables[3])

    row_head = lax.broadcasted_iota(jnp.int32, (per_group * WINDOW, 1), 0) // WINDOW

    def attend_block(layer, q_ref, kv_ref, here, near, near_bias, sink_row, out):
        near_bias = jnp.concatenate([near_bias] * per_group, axis=0)
        for g in range(groups):
            first = g * per_group
            k = kv_ref[near, g * HEAD_DIM : (g + 1) * HEAD_DIM]
            v = kv_ref[near, kv_cols + g * HEAD_DIM : kv_cols + (g + 1) * HEAD_DIM]
            q = jnp.concatenate(
                [q_ref[here, h * HEAD_DIM : (h + 1) * HEAD_DIM] for h in range(first, first + per_group)], axis=0
            )
            scores = lax.dot_general(q, k, (((1,), (1,)), ((), ())), preferred_element_type=F32) + near_bias
            sink = jnp.zeros((per_group * WINDOW, 1), F32)
            for e in range(per_group):
                sink = jnp.where(row_head == e, sink_row[:, first + e : first + e + 1], sink)
            largest = jnp.maximum(jnp.max(scores, axis=-1, keepdims=True), sink)
            powers = jnp.exp(scores - largest)
            total = jnp.sum(powers, axis=-1, keepdims=True) + jnp.exp(sink - largest)
            mixed = jnp.dot(powers.astype(BF16), v, preferred_element_type=F32) * (1.0 / total)
            mixed = mixed.astype(BF16)
            out[here, first * HEAD_DIM : (first + per_group) * HEAD_DIM] = jnp.concatenate(
                [mixed[e * WINDOW : (e + 1) * WINDOW] for e in range(per_group)], axis=1
            )

    def attend0(i):
        if i == 0:
            pl.when(span_low)(lambda: halo(0, 0, True).wait_recv())
        if i == n_tp - 1:
            pl.when(span_high)(lambda: halo(0, 0, False).wait_recv())

        def one(b, carry):
            here = pl.ds(pl.multiple_of(b * WINDOW, WINDOW), WINDOW)
            near = pl.ds(pl.multiple_of(i * tokens + b * WINDOW, WINDOW), reach_of)
            attend_block(0, queries.at[i], kv0, here, near, bias[i * blocks + b], sink_ref[0:1], mine.at[i])
            return carry

        lax.fori_loop(0, blocks, one, 0)

    def slice_copy(i, source):
        to = {"sp": sp, "tp": i}
        return send(mine.at[i], attended.at[source], slice_send.at[i], slice_recv.at[source], to)

    def send_slice(i):
        pl.when(tp != i)(lambda: slice_copy(i, tp).start())

        @pl.when(tp == i)
        def _():
            attended[i] = mine[i]

    def wait_slices():
        for t in range(n_tp):
            pl.when(tp != t)(lambda: slice_copy(t, t).wait_recv())

    def attend(layer, t):
        wait_halo(layer, t)

        def one(b, carry):
            here = pl.ds(pl.multiple_of(b * WINDOW, WINDOW), WINDOW)
            near = pl.ds(pl.multiple_of(b * WINDOW, WINDOW), reach_of)
            attend_block(
                layer, queries.at[t], kv.at[layer - 1, t], here, near, bias[tp * blocks + b],
                sinks[t, layer : layer + 1], attended.at[t],
            )
            return carry

        lax.fori_loop(0, blocks, one, 0)

    def make_state(layer, s):
        piece = jnp.zeros((tokens, rows), F32)
        for t in range(n_tp):
            piece += lax.dot_general(
                attended[t], w[2, layer, t // n_c, t % n_c, s // n_y, s % n_y],
                (((1,), (1,)), ((), ())), preferred_element_type=F32,
            )
        target = out_ref if layer == layers - 1 else state
        target[:, s * rows : (s + 1) * rows] = piece.astype(BF16)

    def sinks_here():
        for k in range(1, n_tp):
            sink_copy(k, True).wait_recv()

    work, costs = [], []

    def add(layer, kind, cost, piece, *where, after=None):
        work.append(functools.partial(piece, *where))
        costs.append((layer, kind, cost, after))
        return len(work) - 1

    for i in range(n_tp):
        add(0, None, 1.1, norm0, i)
    ends_first = [0, n_tp - 1] + list(range(1, n_tp - 1))
    for i in ends_first:
        add(0, 0, 0.85, make_kv0, i)
    sent = add(0, 0, 0.05, send_halo, 0, 0)
    for i in range(n_tp):
        add(0, 1, 0.85, make_q0, i)
    middle_first = list(range(1, n_tp)) + [0]
    for j, i in enumerate(middle_first):
        edge = i in (0, n_tp - 1)
        add(0, 1, 1.3, attend0, i, after=(sent, 5.0) if edge else None)
        if j:
            add(0, 1, 0.05, send_slice, middle_first[j - 1])
    add(0, 1, 0.05, sinks_here)
    sent = add(0, 1, 0.05, send_slice, middle_first[-1])
    add(0, 2, 0.05, wait_slices, after=(sent, 4.0))
    for layer in range(layers):
        if layer:
            add(layer, None, 1.0, norm, layer)
            sent = []
            for t in range(n_tp):
                add(layer, 0, 0.75, make_kv, layer, t)
                if t:
                    sent.append(add(layer, 0, 0.05, send_halo, layer, t - 1))
            for t in range(n_tp):
                add(layer, 1, 0.75, make_q, layer, t)
                if t == 0:
                    sent.append(add(layer, 1, 0.05, send_halo, layer, n_tp - 1))
            for t in range(n_tp):
                add(layer, 1, 1.3, attend, layer, t, after=(sent[t], 5.0))
        for s in range(n_sp):
            add(layer, 2, 0.4, make_state, layer, s)

    missing = {(layer, kind): 0 for layer in range(layers) for kind in (None, 0, 1, 2)}
    for unit in units:
        missing[unit[:2]] += 1

    def compute(budget):
        while work and missing[costs[0][:2]] == 0 and budget > 0:
            work.pop(0)()
            budget -= min(1.0, 2.0 * costs.pop(0)[2])

    def landed(u):
        missing[units[u][:2]] -= 1

    compute(n_tp)
    for s in range(count + LAGS[5] + 1):
        slots = SLOTS if s < LATE_FROM * count else LATE
        if AHEAD <= s + AHEAD < count:
            depart(s + AHEAD)
        for stage in range(3):
            u, v = s - LAGS[2 * stage], s - LAGS[2 * stage + 1]
            if 0 <= u < count:
                pass_on(u, stage)
            if 0 <= v < count:
                advance(v, stage)
                if stage == 1 and len(units[v][4][0]) == 2:
                    landed(v)
            compute(slots[stage])
        u = s - LAGS[5] - 1
        if 0 <= u < count and len(units[u][4][0]) == 3:
            wait_shared(u)
            landed(u)
        compute(slots[3])
        u = s - LAGS[5] - 1 - SETTLE
        if 0 <= u < count:
            drain(u)
    compute(math.inf)

    for u in range(count - SETTLE, count):
        drain(u)
    for k in range(1, n_tp):
        sink_copy(k, False).wait_send()
    for i in range(n_tp):
        pl.when(tp != i)(lambda: slice_copy(i, tp).wait_send())
    for layer in range(layers):
        low, high = low_high(layer)
        for t in range(n_tp if layer else 1):
            pl.when(low)(lambda: halo(layer, t, False).wait_send())
            pl.when(high)(lambda: halo(layer, t, True).wait_send())


def shards(
    grid, inputs, norm_gain, query_weight, key_weight, value_weight, output_weight, sink_logit, final_gain
):
    n_z, n_y, n_x, n_c = grid
    n_sp, n_tp = n_z * n_y, n_x * n_c
    layers, rows, cols = query_weight.shape
    kv_cols = key_weight.shape[2]
    features = inputs.shape[1]
    span = inputs.shape[0]
    tokens = span // n_tp
    units = unit_list(layers, rows)

    half = HEAD_DIM // 2
    inverse = 10000.0 ** (-jnp.arange(half).astype(F32) / half)
    inverse = jnp.tile(inverse, 4)[None]

    if kv_cols % LANES:
        weights = [jnp.concatenate([key_weight, value_weight], axis=2), query_weight, output_weight]
        sources = [(0, 0, cols), (1, 0, cols), (2, 0, cols)]
    else:
        weights = [key_weight, value_weight, query_weight, output_weight]
        sources = [(0, 0, kv_cols), (0, kv_cols, kv_cols), (1, 0, cols), (2, 0, cols)]

    copies = len(units) * (n_z + n_y + n_x - 2 + max(n_z, n_y, n_x))
    vmem = pl.BlockSpec(memory_space=pltpu.VMEM)
    hbm = pl.BlockSpec(memory_space=pl.ANY)
    state = pl.pallas_call(
        functools.partial(stack_kernel, grid, sources, units),
        name="stack",
        out_shape=jax.ShapeDtypeStruct((tokens, features), BF16),
        in_specs=[hbm, vmem, vmem, vmem] + [hbm] * len(weights),
        out_specs=vmem,
        scratch_shapes=[
            pltpu.VMEM((KINDS, layers, n_x, n_c, n_z, n_y, rows, cols), BF16),
            pltpu.VMEM((2, tokens, features), BF16),
            pltpu.VMEM((tokens, features), BF16),
            pltpu.VMEM((n_tp, tokens, features), BF16),
            pltpu.VMEM((n_tp, tokens, cols), BF16),
            pltpu.VMEM((span + 2 * WINDOW, cols), BF16),
            pltpu.VMEM((layers - 1, n_tp, tokens + 2 * WINDOW, cols), BF16),
            pltpu.VMEM((n_tp, tokens, cols), BF16),
            pltpu.VMEM((n_tp, tokens, cols), BF16),
            pltpu.VMEM((span // WINDOW, WINDOW, 3 * WINDOW), F32),
            pltpu.VMEM((span, 2 * HEAD_DIM), F32),
            pltpu.VMEM((4, tokens, cols), F32),
            pltpu.VMEM((n_tp,) + sink_logit.shape, F32),
            pltpu.SemaphoreType.DMA((copies,)),
            pltpu.SemaphoreType.DMA((copies,)),
            pltpu.SemaphoreType.DMA((layers * n_tp * 2,)),
            pltpu.SemaphoreType.DMA((layers * n_tp * 2,)),
            pltpu.SemaphoreType.DMA((n_tp,)),
            pltpu.SemaphoreType.DMA((n_tp,)),
            pltpu.SemaphoreType.DMA((n_tp - 1,)),
            pltpu.SemaphoreType.DMA((n_tp - 1,)),
            pltpu.SemaphoreType.DMA((len(weights) + n_tp,)),
        ],
        compiler_params=pltpu.CompilerParams(
            vmem_limit_bytes=VMEM_LIMIT, collective_id=0, has_side_effects=True
        ),
    )(inputs, norm_gain, sink_logit, inverse, *weights)
    step = min(64, tokens)
    return pl.pallas_call(
        finish_kernel,
        name="finish",
        grid=(tokens // step,),
        out_shape=jax.ShapeDtypeStruct((tokens, features), F32),
        in_specs=[pl.BlockSpec((step, features), lambda i: (i, 0)), pl.BlockSpec((1, features), lambda i: (0, 0))],
        out_specs=pl.BlockSpec((step, features), lambda i: (i, 0)),
    )(state, final_gain[None])


def solution(mesh):
    in_specs = (
        P("sp", None),
        P(),
        P(None, "sp", "tp"),
        P(None, "sp", "tp"),
        P(None, "sp", "tp"),
        P(None, "sp", "tp"),
        P(None, "tp"),
        P(),
    )
    out_specs = P(("sp", "tp"), None)
    return jax.shard_map(
        functools.partial(shards, grid_of(mesh)), mesh=mesh, in_specs=in_specs, out_specs=out_specs, check_vma=False
    )
```

```python
import functools
import math

import jax
import jax.numpy as jnp
from jax import lax
from jax.experimental import pallas as pl
from jax.experimental.pallas import tpu as pltpu
from jax.sharding import PartitionSpec as P

HEAD_DIM = 64
WINDOW = 128
EPS = 1e-06
LANES = 128
F32 = jnp.float32
BF16 = jnp.bfloat16
VMEM_LIMIT = 60 * 1024 * 1024
KINDS = 3
SPLIT = 2
AHEAD = 2
LAGS = (0, 1, 2, 3, 4, 5)
SLOTS = (1, 1, 0, 1)
LATE = (2, 2, 2, 2)
LATE_FROM = 0.75
SETTLE = 2
WHOLE = slice(None)
LINE = 4


def grid_of(mesh):
    n_sp, n_tp = mesh.shape["sp"], mesh.shape["tp"]
    devices = mesh.devices
    n_z = len({d.coords[2] for d in devices[:, 0]})
    n_x = len({d.coords[0] for d in devices[0, :]})
    return n_z, n_sp // n_z, n_x, n_tp // n_x


def unit_list(layers, rows):
    units = []
    n = 0
    for layer in range(layers):
        for kind in range(KINDS):
            pieces = SPLIT * 2 if (layer, kind) == (layers - 1, KINDS - 1) else SPLIT
            size = rows // pieces
            for piece in range(pieces):
                if layer == 0 and kind < 2:
                    orders = (("z", "y"), ("z", "y"))
                else:
                    orders = FLAVOURS[PATTERN[n % len(PATTERN)]]
                    n += 1
                units.append((layer, kind, piece * size, size, orders))
    return units


FLAVOURS = {
    "a": (("z", "y", "x"), ("z", "x", "y")),
    "b": (("y", "z", "x"), ("x", "z", "y")),
    "A": (("z", "y", "x"), ("z", "y", "x")),
    "B": (("y", "z", "x"), ("y", "z", "x")),
    "c": (("y", "x", "z"), ("x", "y", "z")),
    "e": (("z", "y", "x"), ("x", "z", "y")),
    "f": (("y", "z", "x"), ("z", "x", "y")),
}
PATTERN = "Abbabbabbabbab"


def normalize(wide, gain):
    inv_root = lax.rsqrt(jnp.mean(wide * wide, axis=-1, keepdims=True) + EPS)
    return wide * inv_root * gain


def finish_kernel(state_ref, gain_ref, out_ref):
    out_ref[...] = normalize(state_ref[...].astype(F32), gain_ref[...])


def stack_kernel(grid, sources, units, *refs):
    n_z, n_y, n_x, n_c = grid
    n_sp, n_tp = n_z * n_y, n_x * n_c
    (inputs_ref, gain_ref, sink_ref, inverse_ref), refs = refs[:4], refs[4:]
    weight_refs, refs = refs[: len(sources)], refs[len(sources) :]
    out_ref, refs = refs[0], refs[1:]
    w, stage_in, state, normed, queries, kv0, kv, mine, attended, bias, trig, tables, sinks = refs[:13]
    send_sem, recv_sem, halo_send, halo_recv, slice_send, slice_recv, sink_send, sink_recv, local_sem = refs[13:]

    layers, rows, cols = w.shape[1], w.shape[6], w.shape[7]
    tokens, features = state.shape
    span = n_tp * tokens
    heads = cols // HEAD_DIM
    groups = heads // 2
    kv_cols = cols // 2
    per_group = heads // groups
    blocks = tokens // WINDOW

    sp, tp = lax.axis_index("sp"), lax.axis_index("tp")
    place = sp * n_tp + tp
    z, y, x, core = sp // n_y, sp % n_y, tp // n_c, tp % n_c
    at = {"z": z, "y": y, "x": x}
    size = {"z": n_z, "y": n_y, "x": n_x}
    other = 1 - core

    def device(**where):
        to = dict(at, core=core)
        to.update(where)
        return {"sp": to["z"] * n_y + to["y"], "tp": to["x"] * n_c + to["core"]}

    def linear(index):
        return {"sp": index // n_tp, "tp": index % n_tp}

    def send(src, dst, send_at, recv_at, to):
        return pltpu.make_async_remote_copy(
            src_ref=src, dst_ref=dst, send_sem=send_at, recv_sem=recv_at,
            device_id=to, device_id_type=pl.DeviceIdType.MESH,
        )

    base = {"z": 0, "y": n_z - 1, "x": n_z + n_y - 2}
    hops = n_z + n_y + n_x - 3
    per_unit = hops + 1 + max(size.values())

    def relayed(axis):
        return axis == "z" and size[axis] == LINE

    def block(u, colour, **where):
        layer, kind, first, count, _ = units[u]
        spot = dict({"z": z, "y": y, "x": x}, **where)
        return w.at[kind, layer, spot["x"], colour, spot["z"], spot["y"], pl.ds(first, count)]

    def part(u, colour, stage, source):
        order = units[u][4][colour]
        spot = {a: WHOLE for a in order[:stage]}
        spot[order[stage]] = source
        return block(u, colour, **spot)

    def staged(u, colour, stage, k, arriving):
        axis = units[u][4][colour][stage]
        view = part(u, colour, stage, (at[axis] + size[axis] - k) % size[axis] if arriving else at[axis])
        number = u * per_unit + base[axis] + k - 1
        to = device(**{axis: (at[axis] + k) % size[axis]})
        return send(view, view, send_sem.at[number], recv_sem.at[number], to)

    def relay(u, colour, stage, inner):
        source, target = (LINE - 1, 0) if inner == 1 else (0, LINE - 1)
        view = part(u, colour, stage, source)
        number = u * per_unit
        k = (target - source) % LINE
        return send(view, view, send_sem.at[number + hops], recv_sem.at[number + k - 1], device(z=target))

    def shared(u, colour, k):
        axis = units[u][4][colour][2]
        view = part(u, colour, 2, (at[axis] + size[axis] - k) % size[axis])
        number = u * per_unit + hops + 1 + k
        return send(view, view, send_sem.at[number], recv_sem.at[number], device(core=other))

    def outgoing(u, colour, stage, do):
        axis = units[u][4][colour][stage]
        if relayed(axis):
            do(staged(u, colour, stage, 2, False))
            pl.when(z != LINE - 1)(lambda: do(staged(u, colour, stage, 1, False)))
            pl.when(z != 0)(lambda: do(staged(u, colour, stage, 3, False)))
        else:
            for k in range(1, size[axis]):
                do(staged(u, colour, stage, k, False))

    def by_core(do):
        for colour in range(n_c):
            pl.when(core == colour)(functools.partial(do, colour))

    def depart(u):
        by_core(lambda colour: outgoing(u, colour, 0, lambda c: c.start()))

    def pass_on(u, stage):
        def do(colour):
            order = units[u][4][colour]
            if stage < len(order) and relayed(order[stage]):
                staged(u, colour, stage, 2, True).wait_recv()
                for inner in (1, 2):
                    pl.when(z == inner)(lambda: relay(u, colour, stage, inner).start())
        by_core(do)

    def advance(u, stage):
        def do(colour):
            order = units[u][4][colour]
            if stage >= len(order):
                return
            axis = order[stage]
            for k in range(1, size[axis]):
                if not (relayed(axis) and k == 2):
                    staged(u, colour, stage, k, True).wait_recv()
            if stage + 1 < len(order):
                outgoing(u, colour, stage + 1, lambda c: c.start())
            if stage == 1 and len(order) == 3:
                shared(u, colour, 0).start()
            if stage == 2:
                for k in range(1, size[axis]):
                    shared(u, colour, k).start()
        by_core(do)

    def wait_shared(u):
        def do(colour):
            order = units[u][4][1 - colour]
            if len(order) == 3:
                for k in range(size[order[2]]):
                    shared(u, 1 - colour, k).wait_recv()
        by_core(do)

    def drain(u):
        def do(colour):
            order = units[u][4][colour]
            for stage, axis in enumerate(order):
                outgoing(u, colour, stage, lambda c: c.wait_send())
                if relayed(axis):
                    for inner in (1, 2):
                        pl.when(z == inner)(lambda: relay(u, colour, stage, inner).wait_send())
            if len(order) == 3:
                for k in range(size[order[2]]):
                    shared(u, colour, k).wait_send()
        by_core(do)

    own = []
    for i, (kind, offset, width) in enumerate(sources):
        dst = w.at[kind, :, x, core, z, y, :, pl.ds(offset, width)]
        own.append(pltpu.make_async_copy(weight_refs[i], dst, local_sem.at[i]))
    for copy in own:
        copy.start()

    def fetch(i):
        return pltpu.make_async_copy(
            inputs_ref.at[pl.ds(i * tokens, tokens)], stage_in.at[i % 2], local_sem.at[len(sources) + i]
        )

    for i in range(2):
        fetch(i).start()

    barrier = pltpu.get_barrier_semaphore()

    def greet(to):
        pl.semaphore_signal(barrier, inc=1, device_id=to, device_id_type=pl.DeviceIdType.MESH)

    everyone = n_sp * n_tp
    met = [device(**{axis: (at[axis] + k) % size[axis]}) for axis in ("z", "y", "x") for k in range(1, size[axis])]
    met += [{"sp": sp, "tp": (tp + k) % n_tp} for k in range(1, n_tp)]
    met += [linear((place + step) % everyone) for step in (1, everyone - 1)]
    met += [{"sp": (sp + step) % n_sp, "tp": tp} for step in (1, n_sp - 1)]
    for to in met:
        greet(to)
    for copy in own:
        copy.wait()
    pl.semaphore_wait(barrier, len(met))

    count = len(units)
    for u in range(AHEAD):
        depart(u)

    def sink_copy(k, arriving):
        source = (tp + n_tp - k) % n_tp if arriving else tp
        to = {"sp": sp, "tp": (tp + k) % n_tp}
        return send(sink_ref, sinks.at[source], sink_send.at[k - 1], sink_recv.at[k - 1], to)

    for k in range(1, n_tp):
        sink_copy(k, False).start()
    sinks[tp] = sink_ref[...]

    root = HEAD_DIM ** (-0.5)
    scale = float(features) ** (-0.5)

    def fill(i, carry):
        first = sp * span + i * WINDOW
        where = lax.broadcasted_iota(jnp.int32, (WINDOW, 2 * HEAD_DIM), 0) + first
        angles = where.astype(F32) * inverse_ref[...]
        column = lax.broadcasted_iota(jnp.int32, (WINDOW, 2 * HEAD_DIM), 1)
        sine = jnp.sin(angles)
        turned = jnp.where(column < HEAD_DIM + HEAD_DIM // 2, -sine, sine)
        trig[pl.ds(pl.multiple_of(i * WINDOW, WINDOW), WINDOW)] = (
            jnp.where(column < HEAD_DIM, jnp.cos(angles), turned) * scale
        )
        return carry

    lax.fori_loop(0, span // WINDOW, fill, 0)

    def turn_tables(kind, where):
        pair_c, pair_s = trig[where, :HEAD_DIM], trig[where, HEAD_DIM:]
        if kind:
            return jnp.concatenate([pair_c * root] * heads, axis=1), jnp.concatenate([pair_s * root] * heads, axis=1)
        one = jnp.ones((tokens, kv_cols), F32)
        return jnp.concatenate([pair_c] * groups + [one], axis=1), jnp.concatenate([pair_s] * groups + [0 * one], axis=1)

    for kind in range(2):
        tables[2 * kind], tables[2 * kind + 1] = turn_tables(kind, pl.ds(pl.multiple_of(tp * tokens, tokens), tokens))
    reach_of = 3 * WINDOW
    row = lax.broadcasted_iota(jnp.int32, (WINDOW, reach_of), 0)
    reach = lax.broadcasted_iota(jnp.int32, (WINDOW, reach_of), 1) - WINDOW
    for b in range(span // WINDOW):
        key_pos = sp * span + b * WINDOW + reach
        allowed = (jnp.abs(row - reach) <= WINDOW) & (key_pos >= 0) & (key_pos < n_sp * span)
        bias[b] = jnp.where(allowed, 0.0, -jnp.inf).astype(F32)

    has_low, has_high = place > 0, place < everyone - 1
    span_low, span_high = sp > 0, sp < n_sp - 1
    nothing = jnp.zeros((layers - 1, n_tp, WINDOW, cols), BF16)

    @pl.when(jnp.logical_not(has_low))
    def _():
        kv[:, :, :WINDOW] = nothing

    @pl.when(jnp.logical_not(has_high))
    def _():
        kv[:, :, WINDOW + tokens :] = nothing

    @pl.when(jnp.logical_not(span_low))
    def _():
        kv0[:WINDOW] = nothing[0, 0]

    @pl.when(jnp.logical_not(span_high))
    def _():
        kv0[WINDOW + span :] = nothing[0, 0]

    def halo(layer, t, up):
        length = span if layer == 0 else tokens
        here = pl.ds(length, WINDOW) if up else pl.ds(WINDOW, WINDOW)
        there = pl.ds(0, WINDOW) if up else pl.ds(WINDOW + length, WINDOW)
        number = (layer * n_tp + t) * 2 + int(up)
        rows_of = kv0 if layer == 0 else kv.at[layer - 1, t]
        step = 1 if up else -1
        to = {"sp": sp + step, "tp": tp} if layer == 0 else linear(place + step)
        return send(rows_of.at[here], rows_of.at[there], halo_send.at[number], halo_recv.at[number], to)

    def low_high(layer):
        return (span_low, span_high) if layer == 0 else (has_low, has_high)

    def send_halo(layer, t):
        low, high = low_high(layer)
        pl.when(low)(lambda: halo(layer, t, False).start())
        pl.when(high)(lambda: halo(layer, t, True).start())

    def wait_halo(layer, t):
        low, high = low_high(layer)
        pl.when(low)(lambda: halo(layer, t, True).wait_recv())
        pl.when(high)(lambda: halo(layer, t, False).wait_recv())

    def norm0(i):
        fetch(i).wait()
        normed[i] = normalize(stage_in[i % 2].astype(F32), gain_ref[0:1]).astype(BF16)
        if i + 2 < n_tp:
            fetch(i + 2).start()

    def norm(layer):
        normed[0] = normalize(state[...].astype(F32), gain_ref[layer : layer + 1]).astype(BF16)

    lane = lax.broadcasted_iota(jnp.int32, (tokens, cols), 1)
    front = (lane % HEAD_DIM) < HEAD_DIM // 2

    def project(chunk, weight, cos_table, sin_table):
        acc = jnp.dot(normed[chunk], weight.reshape(features, cols), preferred_element_type=F32)
        step = HEAD_DIM // 2
        partner = jnp.where(front, pltpu.roll(acc, cols - step, 1), pltpu.roll(acc, step, 1))
        return (acc * cos_table + partner * sin_table).astype(BF16)

    def make_kv0(i):
        kv0[WINDOW + i * tokens : WINDOW + (i + 1) * tokens] = project(
            i, w[0, 0, x, core], *turn_tables(0, pl.ds(i * tokens, tokens))
        )

    def make_q0(i):
        queries[i] = project(i, w[1, 0, x, core], *turn_tables(1, pl.ds(i * tokens, tokens)))

    def make_kv(layer, t):
        kv[layer - 1, t, WINDOW : WINDOW + tokens] = project(0, w[0, layer, t // n_c, t % n_c], tables[0], tables[1])

    def make_q(layer, t):
        queries[t] = project(0, w[1, layer, t // n_c, t % n_c], tables[2], tables[3])

    row_head = lax.broadcasted_iota(jnp.int32, (per_group * WINDOW, 1), 0) // WINDOW

    def attend_block(layer, q_ref, kv_ref, here, near, near_bias, sink_row, out):
        near_bias = jnp.concatenate([near_bias] * per_group, axis=0)
        for g in range(groups):
            first = g * per_group
            k = kv_ref[near, g * HEAD_DIM : (g + 1) * HEAD_DIM]
            v = kv_ref[near, kv_cols + g * HEAD_DIM : kv_cols + (g + 1) * HEAD_DIM]
            q = jnp.concatenate(
                [q_ref[here, h * HEAD_DIM : (h + 1) * HEAD_DIM] for h in range(first, first + per_group)], axis=0
            )
            scores = lax.dot_general(q, k, (((1,), (1,)), ((), ())), preferred_element_type=F32) + near_bias
            sink = jnp.zeros((per_group * WINDOW, 1), F32)
            for e in range(per_group):
                sink = jnp.where(row_head == e, sink_row[:, first + e : first + e + 1], sink)
            largest = jnp.maximum(jnp.max(scores, axis=-1, keepdims=True), sink)
            powers = jnp.exp(scores - largest)
            total = jnp.sum(powers, axis=-1, keepdims=True) + jnp.exp(sink - largest)
            mixed = jnp.dot(powers.astype(BF16), v, preferred_element_type=F32) * (1.0 / total)
            mixed = mixed.astype(BF16)
            out[here, first * HEAD_DIM : (first + per_group) * HEAD_DIM] = jnp.concatenate(
                [mixed[e * WINDOW : (e + 1) * WINDOW] for e in range(per_group)], axis=1
            )

    def attend0(i):
        if i == 0:
            pl.when(span_low)(lambda: halo(0, 0, True).wait_recv())
        if i == n_tp - 1:
            pl.when(span_high)(lambda: halo(0, 0, False).wait_recv())

        def one(b, carry):
            here = pl.ds(pl.multiple_of(b * WINDOW, WINDOW), WINDOW)
            near = pl.ds(pl.multiple_of(i * tokens + b * WINDOW, WINDOW), reach_of)
            attend_block(0, queries.at[i], kv0, here, near, bias[i * blocks + b], sink_ref[0:1], mine.at[i])
            return carry

        lax.fori_loop(0, blocks, one, 0)

    def slice_copy(i, source):
        to = {"sp": sp, "tp": i}
        return send(mine.at[i], attended.at[source], slice_send.at[i], slice_recv.at[source], to)

    def send_slice(i):
        pl.when(tp != i)(lambda: slice_copy(i, tp).start())

        @pl.when(tp == i)
        def _():
            attended[i] = mine[i]

    def wait_slices():
        for t in range(n_tp):
            pl.when(tp != t)(lambda: slice_copy(t, t).wait_recv())

    def attend(layer, t):
        wait_halo(layer, t)

        def one(b, carry):
            here = pl.ds(pl.multiple_of(b * WINDOW, WINDOW), WINDOW)
            near = pl.ds(pl.multiple_of(b * WINDOW, WINDOW), reach_of)
            attend_block(
                layer, queries.at[t], kv.at[layer - 1, t], here, near, bias[tp * blocks + b],
                sinks[t, layer : layer + 1], attended.at[t],
            )
            return carry

        lax.fori_loop(0, blocks, one, 0)

    def make_state(layer, s):
        piece = jnp.zeros((tokens, rows), F32)
        for t in range(n_tp):
            piece += lax.dot_general(
                attended[t], w[2, layer, t // n_c, t % n_c, s // n_y, s % n_y],
                (((1,), (1,)), ((), ())), preferred_element_type=F32,
            )
        target = out_ref if layer == layers - 1 else state
        target[:, s * rows : (s + 1) * rows] = piece.astype(BF16)

    def sinks_here():
        for k in range(1, n_tp):
            sink_copy(k, True).wait_recv()

    work, costs = [], []

    def add(layer, kind, cost, piece, *where, after=None):
        work.append(functools.partial(piece, *where))
        costs.append((layer, kind, cost, after))
        return len(work) - 1

    for i in range(n_tp):
        add(0, None, 1.1, norm0, i)
    ends_first = [0, n_tp - 1] + list(range(1, n_tp - 1))
    for i in ends_first:
        add(0, 0, 0.85, make_kv0, i)
    sent = add(0, 0, 0.05, send_halo, 0, 0)
    for i in range(n_tp):
        add(0, 1, 0.85, make_q0, i)
    middle_first = list(range(1, n_tp)) + [0]
    for j, i in enumerate(middle_first):
        edge = i in (0, n_tp - 1)
        add(0, 1, 1.3, attend0, i, after=(sent, 5.0) if edge else None)
        if j:
            add(0, 1, 0.05, send_slice, middle_first[j - 1])
    add(0, 1, 0.05, sinks_here)
    sent = add(0, 1, 0.05, send_slice, middle_first[-1])
    add(0, 2, 0.05, wait_slices, after=(sent, 4.0))
    for layer in range(layers):
        if layer:
            add(layer, None, 1.0, norm, layer)
            sent = []
            for t in range(n_tp):
                add(layer, 0, 0.75, make_kv, layer, t)
                if t:
                    sent.append(add(layer, 0, 0.05, send_halo, layer, t - 1))
            for t in range(n_tp):
                add(layer, 1, 0.75, make_q, layer, t)
                if t == 0:
                    sent.append(add(layer, 1, 0.05, send_halo, layer, n_tp - 1))
            for t in range(n_tp):
                add(layer, 1, 1.3, attend, layer, t, after=(sent[t], 5.0))
        for s in range(n_sp):
            add(layer, 2, 0.4, make_state, layer, s)

    missing = {(layer, kind): 0 for layer in range(layers) for kind in (None, 0, 1, 2)}
    for unit in units:
        missing[unit[:2]] += 1

    def compute(budget):
        while work and missing[costs[0][:2]] == 0 and budget > 0:
            work.pop(0)()
            budget -= min(1.0, 2.0 * costs.pop(0)[2])

    def landed(u):
        missing[units[u][:2]] -= 1

    compute(n_tp)
    for s in range(count + LAGS[5] + 1):
        slots = SLOTS if s < LATE_FROM * count else LATE
        if AHEAD <= s + AHEAD < count:
            depart(s + AHEAD)
        for stage in range(3):
            u, v = s - LAGS[2 * stage], s - LAGS[2 * stage + 1]
            if 0 <= u < count:
                pass_on(u, stage)
            if 0 <= v < count:
                advance(v, stage)
                if stage == 1 and len(units[v][4][0]) == 2:
                    landed(v)
            compute(slots[stage])
        u = s - LAGS[5] - 1
        if 0 <= u < count and len(units[u][4][0]) == 3:
            wait_shared(u)
            landed(u)
        compute(slots[3])
        u = s - LAGS[5] - 1 - SETTLE
        if 0 <= u < count:
            drain(u)
    compute(math.inf)

    for u in range(count - SETTLE, count):
        drain(u)
    for k in range(1, n_tp):
        sink_copy(k, False).wait_send()
    for i in range(n_tp):
        pl.when(tp != i)(lambda: slice_copy(i, tp).wait_send())
    for layer in range(layers):
        low, high = low_high(layer)
        for t in range(n_tp if layer else 1):
            pl.when(low)(lambda: halo(layer, t, False).wait_send())
            pl.when(high)(lambda: halo(layer, t, True).wait_send())


def shards(
    grid, inputs, norm_gain, query_weight, key_weight, value_weight, output_weight, sink_logit, final_gain
):
    n_z, n_y, n_x, n_c = grid
    n_sp, n_tp = n_z * n_y, n_x * n_c
    layers, rows, cols = query_weight.shape
    kv_cols = key_weight.shape[2]
    features = inputs.shape[1]
    span = inputs.shape[0]
    tokens = span // n_tp
    units = unit_list(layers, rows)

    half = HEAD_DIM // 2
    inverse = 10000.0 ** (-jnp.arange(half).astype(F32) / half)
    inverse = jnp.tile(inverse, 4)[None]

    if kv_cols % LANES:
        weights = [jnp.concatenate([key_weight, value_weight], axis=2), query_weight, output_weight]
        sources = [(0, 0, cols), (1, 0, cols), (2, 0, cols)]
    else:
        weights = [key_weight, value_weight, query_weight, output_weight]
        sources = [(0, 0, kv_cols), (0, kv_cols, kv_cols), (1, 0, cols), (2, 0, cols)]

    copies = len(units) * (n_z + n_y + n_x - 2 + max(n_z, n_y, n_x))
    vmem = pl.BlockSpec(memory_space=pltpu.VMEM)
    hbm = pl.BlockSpec(memory_space=pl.ANY)
    state = pl.pallas_call(
        functools.partial(stack_kernel, grid, sources, units),
        name="stack",
        out_shape=jax.ShapeDtypeStruct((tokens, features), BF16),
        in_specs=[hbm, vmem, vmem, vmem] + [hbm] * len(weights),
        out_specs=vmem,
        scratch_shapes=[
            pltpu.VMEM((KINDS, layers, n_x, n_c, n_z, n_y, rows, cols), BF16),
            pltpu.VMEM((2, tokens, features), BF16),
            pltpu.VMEM((tokens, features), BF16),
            pltpu.VMEM((n_tp, tokens, features), BF16),
            pltpu.VMEM((n_tp, tokens, cols), BF16),
            pltpu.VMEM((span + 2 * WINDOW, cols), BF16),
            pltpu.VMEM((layers - 1, n_tp, tokens + 2 * WINDOW, cols), BF16),
            pltpu.VMEM((n_tp, tokens, cols), BF16),
            pltpu.VMEM((n_tp, tokens, cols), BF16),
            pltpu.VMEM((span // WINDOW, WINDOW, 3 * WINDOW), F32),
            pltpu.VMEM((span, 2 * HEAD_DIM), F32),
            pltpu.VMEM((4, tokens, cols), F32),
            pltpu.VMEM((n_tp,) + sink_logit.shape, F32),
            pltpu.SemaphoreType.DMA((copies,)),
            pltpu.SemaphoreType.DMA((copies,)),
            pltpu.SemaphoreType.DMA((layers * n_tp * 2,)),
            pltpu.SemaphoreType.DMA((layers * n_tp * 2,)),
            pltpu.SemaphoreType.DMA((n_tp,)),
            pltpu.SemaphoreType.DMA((n_tp,)),
            pltpu.SemaphoreType.DMA((n_tp - 1,)),
            pltpu.SemaphoreType.DMA((n_tp - 1,)),
            pltpu.SemaphoreType.DMA((len(weights) + n_tp,)),
        ],
        compiler_params=pltpu.CompilerParams(
            vmem_limit_bytes=VMEM_LIMIT, collective_id=0, has_side_effects=True
        ),
    )(inputs, norm_gain, sink_logit, inverse, *weights)
    step = min(64, tokens)
    return pl.pallas_call(
        finish_kernel,
        name="finish",
        grid=(tokens // step,),
        out_shape=jax.ShapeDtypeStruct((tokens, features), F32),
        in_specs=[pl.BlockSpec((step, features), lambda i: (i, 0)), pl.BlockSpec((1, features), lambda i: (0, 0))],
        out_specs=pl.BlockSpec((step, features), lambda i: (i, 0)),
    )(state, final_gain[None])


def solution(mesh):
    in_specs = (
        P("sp", None),
        P(),
        P(None, "sp", "tp"),
        P(None, "sp", "tp"),
        P(None, "sp", "tp"),
        P(None, "sp", "tp"),
        P(None, "tp"),
        P(),
    )
    out_specs = P(("sp", "tp"), None)
    return jax.shard_map(
        functools.partial(shards, grid_of(mesh)), mesh=mesh, in_specs=in_specs, out_specs=out_specs, check_vma=False
    )
```
